32 devices in a mesh: fs: 8 (over z, y), tp: 4 (over x, core).
Axes of the slice: x: 2, y: 2, z: 4, core: 2. Of those that a mesh axis runs over, the one named last changes fastest.
Arguments:
- inputs: bfloat16 [9216, 2048], P('fs'), may hold values from -6 to 6
- gate_cot: bfloat16 [9216, 4096], P('fs', 'tp'), may hold values from -0.0546875 to 0.0546875
- state_cot: bfloat16 [9216, 1024], P('fs', 'tp'), may hold values from -0.0546875 to 0.0546875
- gate_weight: float32 [2048, 4096], P('fs', 'tp'), may hold values from -0.75 to 0.75
- state_weight: float32 [2048, 1024], P('fs', 'tp'), may hold values from -0.75 to 0.75
- gate_factor: bfloat16 [2048, 256], P('fs'), may hold values from -0.375 to 0.375
- state_factor: bfloat16 [2048, 256], P('fs'), may hold values from -0.375 to 0.375
- gate_first: float32 [256, 4096], P('fs', 'tp'), may hold values from -6 to 6
- gate_second: float32 [256, 4096], P('fs', 'tp'), may hold values from 0.3 to 3
- state_first: float32 [256, 1024], P('fs', 'tp'), may hold values from -6 to 6
- state_second: float32 [256, 1024], P('fs', 'tp'), may hold values from 0.3 to 3
Outputs:
- new_gate_weight: float32 [2048, 4096], P('fs', 'tp')
- new_state_weight: float32 [2048, 1024], P('fs', 'tp')
- gate_copy: bfloat16 [2048, 4096], P(None, 'tp')
- state_copy: bfloat16 [2048, 1024], P(None, 'tp')
- new_gate_first: float32 [256, 4096], P('fs', 'tp')
- new_gate_second: float32 [256, 4096], P('fs', 'tp')
- new_state_first: float32 [256, 1024], P('fs', 'tp')
- new_state_second: float32 [256, 1024], P('fs', 'tp')
The draws below stay inside these ranges and needn't reach their ends.
All inputs are finite; a program needn't handle non-finite values.
Results may differ from the reference program's by a relative error of at most 0.004.
Values may be sent and summed in bfloat16 or wider, within the bound.
No kernel may reach another device: no remote copies, remote signals or barrier semaphores. Data moves between devices by JAX's collectives and lax.ppermute only.
A program may use at most 128 MiB of HBM per device.

```python
import math
import jax
import jax.numpy as jnp
from jax import lax

D = 2048
DI = 4096
BW = 1024
RANK = 256
TOK_DEV = 1152
TOKENS = 9216
N_FS = 8


def block_levels(rng, shape, split, low, largest):
    level = 1.0
    for position, parts in split:
        heights = jax.random.uniform(jax.random.fold_in(jax.random.fold_in(rng, 6), position), (parts,), jnp.float32, low / len(split), largest / len(split))
        level = level * jnp.repeat(jnp.exp(heights), shape[position] // parts).reshape((-1,) + (1,) * (len(shape) - 1 - position))
    return level


def centred(own_key, dims, width, limit, shards=(), kind=jnp.bfloat16):
    result = jax.random.normal(own_key, dims, jnp.float32) * width
    if len(shards) > 0:
        result = block_levels(own_key, dims, shards, -0.22, 0.18) * result
    return jnp.clip(result, min=-limit, max=limit).astype(kind)


def setup_inputs(seed: int = 0) -> dict:
    arg_keys = jax.random.split(jax.random.key(seed), 12)
    inputs = centred(arg_keys[0], (TOKENS, D), 1.0, 6.0, ((0, 8),))
    gate_cot = centred(arg_keys[1], (TOKENS, DI), (0.35 / (TOK_DEV * N_FS) ** 0.5), 0.0546875, ((0, 8), (1, 4)))
    state_cot = centred(arg_keys[2], (TOKENS, BW), (0.35 / (TOK_DEV * N_FS) ** 0.5), 0.0546875, ((0, 8), (1, 4)))
    gate_weight = centred(arg_keys[3], (D, DI), 0.05, 0.75, ((0, 8), (1, 4)), jnp.float32)
    state_weight = centred(arg_keys[4], (D, BW), 0.05, 0.75, ((0, 8), (1, 4)), jnp.float32)
    gate_factor = centred(arg_keys[5], (D, RANK), RANK ** -0.5, 0.375, ((0, 8),))
    state_factor = centred(arg_keys[6], (D, RANK), RANK ** -0.5, 0.375, ((0, 8),))
    gate_first = centred(arg_keys[7], (RANK, DI), 1.0, 6.0, ((0, 8), (1, 4)), jnp.float32)
    gate_second = jnp.clip(jnp.exp(math.log(3.0) - 2.3025851 * jax.random.uniform(arg_keys[8], (RANK, DI), jnp.float32) ** block_levels(arg_keys[8], (RANK, DI), ((0, 8), (1, 4)), -0.2, 0.2)), 0.3, 3.0)
    state_first = centred(arg_keys[9], (RANK, BW), 1.0, 6.0, ((0, 8), (1, 4)), jnp.float32)
    state_second = jnp.clip(jnp.exp(math.log(3.0) - 2.3025851 * jax.random.uniform(arg_keys[10], (RANK, BW), jnp.float32) ** block_levels(arg_keys[10], (RANK, BW), ((0, 8), (1, 4)), -0.2, 0.2)), 0.3, 3.0)
    return dict(inputs=inputs, gate_cot=gate_cot, state_cot=state_cot, gate_weight=gate_weight, state_weight=state_weight, gate_factor=gate_factor, state_factor=state_factor, gate_first=gate_first, gate_second=gate_second, state_first=state_first, state_second=state_second)


def update_one(inputs, cot, weight, factor, first, second):
    inputs_wide = inputs.astype(jnp.float32)
    factor_wide = factor.astype(jnp.float32)
    lifted = jnp.dot(inputs_wide, factor_wide, precision=lax.Precision.HIGHEST)
    proj = jnp.dot(lifted.T, cot.astype(jnp.float32), precision=lax.Precision.HIGHEST)
    first_new = 0.8 * first + 0.2 * proj
    second_new = 0.9 * second + 0.1 * proj * proj
    direction = (first_new / jnp.sqrt(second_new)).astype(jnp.bfloat16)
    full = jnp.dot(factor_wide, direction.astype(jnp.float32), precision=lax.Precision.HIGHEST)
    scale = 0.02 / jnp.sqrt(jnp.mean(full * full) + 0.25)
    updated = weight - scale * full
    return (updated, updated.astype(jnp.bfloat16), first_new, second_new)

def reference(inputs, gate_cot, state_cot, gate_weight, state_weight, gate_factor, state_factor, gate_first, gate_second, state_first, state_second):
    gate_new, gate_copy, gate_first_new, gate_second_new = update_one(inputs, gate_cot, gate_weight, gate_factor, gate_first, gate_second)
    state_new, state_copy, state_first_new, state_second_new = update_one(inputs, state_cot, state_weight, state_factor, state_first, state_second)
    return (gate_new, state_new, gate_copy, state_copy, gate_first_new, gate_second_new, state_first_new, state_second_new)
```

```python
import jax
import jax.numpy as jnp
from jax import lax
from jax.sharding import PartitionSpec as P

BF = jnp.bfloat16
F32 = jnp.float32


def hop(value, axis, size, step):
    return lax.ppermute(value, axis, [(i, i ^ step) for i in range(size)])


def place(buffer, value, index):
    return lax.dynamic_update_index_in_dim(buffer, value, index, 0)


def by_blocks(blocks, count):
    def build(me):
        first = next(iter(blocks.values()))
        whole = jnp.zeros((count,) + first.shape, first.dtype)
        for step, block in blocks.items():
            whole = place(whole, block, me ^ step)
        return whole

    return build


def quick(n_fs, n_tp):
    def per_device(
        inputs, gate_cot, state_cot, gate_weight, state_weight, gate_factor, state_factor,
        gate_first, gate_second, state_first, state_second,
    ):
        fs = lax.axis_index("fs")
        tp = lax.axis_index("tp")
        rows = gate_factor.shape[0]
        rank = gate_factor.shape[1]
        tokens = inputs.shape[0]
        gate_cols = gate_cot.shape[1]
        state_cols = state_cot.shape[1]
        cols = gate_cols + state_cols
        quarter = 2 * rank // n_tp
        half = n_tp // 2
        own_rows = rank // n_fs

        factors = jnp.concatenate([gate_factor, state_factor], 1)
        mine = lax.dynamic_slice_in_dim(factors, tp * quarter, quarter, 1)
        got = {0: mine}
        for step in range(1, n_fs):
            got[step] = hop(mine, "fs", n_fs, step)
        part = by_blocks(got, n_fs)(fs).reshape(n_fs * rows, quarter)

        own_weight = jnp.concatenate([gate_weight.astype(BF), state_weight.astype(BF)], 1)
        own_weight, part = lax.optimization_barrier((own_weight, part))
        weights = {0: own_weight}
        for step in range(2, n_fs, 2):
            weights[step] = hop(own_weight, "fs", n_fs, step)
        for step in range(0, n_fs, 2):
            weights[step + 1] = hop(weights[step], "fs", n_fs, 1)

        lifted = jnp.dot(inputs, part, preferred_element_type=F32).astype(BF)
        spread = {0: lifted}
        factor_parts = {0: part}
        step = half
        while step:
            for known in list(spread):
                spread[known ^ step] = hop(spread[known], "tp", n_tp, step)
            step //= 2
        lifts = by_blocks(spread, n_tp)(tp)

        gate_part = jnp.einsum("atr,tc->arc", lifts[:half], gate_cot, preferred_element_type=F32)
        state_part = jnp.einsum("atr,tc->arc", lifts[half:], state_cot, preferred_element_type=F32)
        partial = jnp.concatenate(
            [gate_part.reshape(n_fs, own_rows, gate_cols), state_part.reshape(n_fs, own_rows, state_cols)], 2
        )
        narrow = partial.astype(BF)
        projection = lax.dynamic_index_in_dim(partial, fs, 0, keepdims=False)
        for step in range(1, n_fs):
            sent = lax.dynamic_index_in_dim(narrow, fs ^ step, 0, keepdims=False)
            projection = projection + hop(sent, "fs", n_fs, step).astype(F32)

        def moments(first, second, proj):
            first_new = 0.8 * first + 0.2 * proj
            second_new = 0.9 * second + 0.1 * proj * proj
            return first_new, second_new, (first_new / jnp.sqrt(second_new)).astype(BF)

        gate_first_new, gate_second_new, gate_dir = moments(gate_first, gate_second, projection[:, :gate_cols])
        state_first_new, state_second_new, state_dir = moments(state_first, state_second, projection[:, gate_cols:])
        direction = jnp.concatenate([gate_dir, state_dir], 1)
        got = {0: direction}
        for step in range(1, n_fs):
            got[step] = hop(direction, "fs", n_fs, step)

        step = half
        while step:
            for known in list(factor_parts):
                factor_parts[known ^ step] = hop(factor_parts[known], "tp", n_tp, step)
            step //= 2
        all_parts = by_blocks(factor_parts, n_tp)(tp)

        dirs = by_blocks(got, n_fs)(fs).reshape(half, quarter, cols) if half * quarter == rank else None
        gate_dirs = dirs[:, :, :gate_cols]
        state_dirs = dirs[:, :, gate_cols:]
        gate_full = jnp.einsum("akr,arc->kc", all_parts[:half], gate_dirs, preferred_element_type=F32)
        state_full = jnp.einsum("akr,arc->kc", all_parts[half:], state_dirs, preferred_element_type=F32)
        squares = jnp.stack([jnp.sum(gate_full * gate_full), jnp.sum(state_full * state_full)])
        step = half
        while step:
            squares = squares + hop(squares, "tp", n_tp, step)
            step //= 2
        d = n_fs * rows
        gate_scale = 0.02 / jnp.sqrt(squares[0] / (d * gate_cols * n_tp) + 0.25)
        state_scale = 0.02 / jnp.sqrt(squares[1] / (d * state_cols * n_tp) + 0.25)

        all_weights = by_blocks(weights, n_fs)(fs).reshape(d, cols)
        gate_copy = (all_weights[:, :gate_cols].astype(F32) - gate_scale * gate_full).astype(BF)
        state_copy = (all_weights[:, gate_cols:].astype(F32) - state_scale * state_full).astype(BF)
        gate_own = jnp.dot(gate_factor, gate_dirs.reshape(rank, gate_cols), preferred_element_type=F32)
        state_own = jnp.dot(state_factor, state_dirs.reshape(rank, state_cols), preferred_element_type=F32)
        gate_new = gate_weight - gate_scale * gate_own
        state_new = state_weight - state_scale * state_own
        return (
            gate_new, state_new, gate_copy, state_copy,
            gate_first_new, gate_second_new, state_first_new, state_second_new,
        )

    return per_device


def plain(n_fs, n_tp):
    def per_device(
        inputs, gate_cot, state_cot, gate_weight, state_weight, gate_factor, state_factor,
        gate_first, gate_second, state_first, state_second,
    ):
        def update(cot, weight, factor, first, second):
            whole = lax.all_gather(factor, "fs", axis=0, tiled=True)
            lifted = jnp.dot(inputs, whole, preferred_element_type=F32)
            upper = lifted.astype(BF)
            lower = (lifted - upper.astype(F32)).astype(BF)
            part = jnp.einsum("tr,tc->rc", upper, cot, preferred_element_type=F32)
            part = part + jnp.einsum("tr,tc->rc", lower, cot, preferred_element_type=F32)
            proj = lax.psum_scatter(part, "fs", scatter_dimension=0, tiled=True)
            first_new = 0.8 * first + 0.2 * proj
            second_new = 0.9 * second + 0.1 * proj * proj
            direction = (first_new / jnp.sqrt(second_new)).astype(BF)
            dirs = lax.all_gather(direction, "fs", axis=0, tiled=True)
            full = jnp.dot(factor, dirs, preferred_element_type=F32)
            square = lax.psum(jnp.sum(full * full), ("fs", "tp"))
            entries = full.shape[0] * full.shape[1] * n_fs * n_tp
            new = weight - 0.02 / jnp.sqrt(square / entries + 0.25) * full
            return new, lax.all_gather(new.astype(BF), "fs", axis=0, tiled=True), first_new, second_new

        g_new, g_copy, g_first, g_second = update(gate_cot, gate_weight, gate_factor, gate_first, gate_second)
        s_new, s_copy, s_first, s_second = update(state_cot, state_weight, state_factor, state_first, state_second)
        return g_new, s_new, g_copy, s_copy, g_first, g_second, s_first, s_second

    return per_device


def solution(mesh):
    n_fs = mesh.shape["fs"]
    n_tp = mesh.shape["tp"]
    small = n_fs in (2, 4, 8) and n_tp in (2, 4)
    both = P("fs", "tp")
    rows = P("fs", None)
    whole = P(None, "tp")
    return jax.shard_map(
        (quick if small else plain)(n_fs, n_tp),
        mesh=mesh,
        in_specs=(rows, both, both, both, both, rows, rows, both, both, both, both),
        out_specs=(both, both, whole, whole, both, both, both, both),
        check_vma=False,
    )
```

```python
import jax
import jax.numpy as jnp
from jax import lax
from jax.experimental import pallas as pl
from jax.experimental.pallas import tpu as pltpu
from jax.sharding import PartitionSpec as P

BF = jnp.bfloat16
F32 = jnp.float32


def hop(value, axis, size, step):
    return lax.ppermute(value, axis, [(i, i ^ step) for i in range(size)])


def place(buffer, value, index):
    return lax.dynamic_update_index_in_dim(buffer, value, index, 0)


def by_blocks(blocks, count):
    def build(me):
        first = next(iter(blocks.values()))
        whole = jnp.zeros((count,) + first.shape, first.dtype)
        for step, block in blocks.items():
            whole = place(whole, block, me ^ step)
        return whole

    return build


VMEM = pl.BlockSpec(memory_space=pltpu.VMEM)
ANY = pl.BlockSpec(memory_space=pl.ANY)
SMEM = pl.BlockSpec(memory_space=pltpu.SMEM)


def lift(order, inputs, pieces):
    n = len(pieces)
    rows, width = pieces[0].shape
    tokens = inputs.shape[0]

    def body(order_ref, inputs_ref, *refs):
        for k in range(n):
            start = pl.multiple_of(order_ref[k] * rows, rows)
            refs[n + 1][pl.ds(start, rows), :] = refs[k][...]
        lifted = jnp.dot(inputs_ref[...], refs[n + 1][...], preferred_element_type=F32)
        refs[n][...] = lifted.T.astype(BF)

    return pl.pallas_call(
        body,
        in_specs=[SMEM, VMEM] + [VMEM] * n,
        out_specs=[VMEM, VMEM],
        out_shape=[jax.ShapeDtypeStruct((width, tokens), BF), jax.ShapeDtypeStruct((n * rows, width), BF)],
        name="lift",
    )(order, inputs, *pieces)


def joined(parts_ref, low, high, rows):
    return jnp.concatenate([parts_ref[p, rows, :] for p in range(low, high)], 1)


def square_sums(order, parts, dirs, gate_cols, rows):
    n_parts = len(parts)
    total, width = parts[0].shape
    half = n_parts // 2

    def body(order_ref, dirs_ref, *refs):
        out_ref, parts_ref = refs[n_parts:]
        for p in range(n_parts):
            parts_ref[order_ref[p]] = refs[p][...]

        def total_of(low, high, cols):
            acc = jnp.zeros((1, dirs_ref[:, cols].shape[1]), F32)
            for r in range(0, total, rows):
                full = jnp.dot(
                    joined(parts_ref, low, high, pl.ds(r, rows)), dirs_ref[:, cols], preferred_element_type=F32
                )
                acc = acc + jnp.sum(full * full, axis=0, keepdims=True)
            return jnp.sum(acc)

        gate = total_of(0, half, slice(0, gate_cols))
        state = total_of(half, n_parts, slice(gate_cols, dirs_ref.shape[1]))
        row = lax.broadcasted_iota(jnp.int32, out_ref.shape, 0)
        out_ref[...] = jnp.where(row < 4, gate, state)

    return pl.pallas_call(
        body,
        in_specs=[SMEM, VMEM] + [VMEM] * n_parts,
        out_specs=[VMEM, VMEM],
        out_shape=[jax.ShapeDtypeStruct((8, 128), F32), jax.ShapeDtypeStruct((n_parts, total, width), BF)],
        name="square_sums",
    )(order, dirs, *parts)


def apply_update(order, sums, parts, dirs, gate_weight, state_weight, weights, pieces, entries):
    n = order.shape[0]
    n_sums = len(sums)
    n_parts = parts.shape[0]
    half = n_parts // 2
    rows, gate_cols = gate_weight.shape
    state_cols = state_weight.shape[1]

    def body(*refs):
        order_ref, refs = refs[0], refs[1:]
        sum_refs, refs = refs[:n_sums], refs[n_sums:]
        parts_ref, dirs_ref, gate_ref, state_ref = refs[:4]
        weights_ref, piece_refs, refs = refs[4], refs[5 : 5 + n], refs[5 + n :]
        gate_new, state_new, gate_copy, state_copy = refs[:4]
        piece_buf, gate_buf, state_buf, gate_out, state_out, gate_own, state_own, sem_in, sem_own, sem_g, sem_s = refs[4:]
        own_in = [
            pltpu.make_async_copy(gate_ref, gate_buf, sem_own.at[0]),
            pltpu.make_async_copy(state_ref, state_buf, sem_own.at[1]),
        ]
        places = [pl.ds(pl.multiple_of(order_ref[k] * rows, rows), rows) for k in range(n)]
        loads = [pltpu.make_async_copy(weights_ref.at[places[k]], piece_buf.at[k], sem_in.at[k]) for k in range(n)]
        for copy in loads[:1] + own_in + loads[1:]:
            copy.start()
        total = sum_refs[0][...] + sum_refs[1][...]
        if n_sums == 4:
            total = total + (sum_refs[2][...] + sum_refs[3][...])
        gate_scale = 0.02 / jnp.sqrt(total[0:1, 0:1] / entries[0] + 0.25)
        state_scale = 0.02 / jnp.sqrt(total[4:5, 0:1] / entries[1] + 0.25)
        stores = []
        for k in range(n):
            at = places[k]
            gate_step = gate_scale * jnp.dot(
                joined(parts_ref, 0, half, at), dirs_ref[:, :gate_cols], preferred_element_type=F32
            )
            state_step = state_scale * jnp.dot(
                joined(parts_ref, half, n_parts, at), dirs_ref[:, gate_cols:], preferred_element_type=F32
            )
            loads[k].wait()
            gate_out[k] = (piece_buf[k].astype(F32) - gate_step).astype(BF)
            state_out[k] = (piece_refs[k][...].astype(F32) - state_step).astype(BF)
            new = [
                pltpu.make_async_copy(gate_out.at[k], gate_copy.at[at], sem_g.at[k]),
                pltpu.make_async_copy(state_out.at[k], state_copy.at[at], sem_s.at[k]),
            ]
            if k == 0:
                for copy in own_in:
                    copy.wait()
                gate_own[...] = gate_buf[...] - gate_step
                state_own[...] = state_buf[...] - state_step
                new.append(pltpu.make_async_copy(gate_own, gate_new, sem_own.at[2]))
                new.append(pltpu.make_async_copy(state_own, state_new, sem_own.at[3]))
            for copy in new:
                copy.start()
            stores += new
        for copy in stores:
            copy.wait()

    return pl.pallas_call(
        body,
        in_specs=[SMEM] + [VMEM] * n_sums + [VMEM, VMEM, ANY, ANY, ANY] + [VMEM] * n,
        out_specs=[ANY] * 4,
        out_shape=[
            jax.ShapeDtypeStruct((rows, gate_cols), F32),
            jax.ShapeDtypeStruct((rows, state_cols), F32),
            jax.ShapeDtypeStruct((n * rows, gate_cols), BF),
            jax.ShapeDtypeStruct((n * rows, state_cols), BF),
        ],
        scratch_shapes=[
            pltpu.VMEM((n, rows, gate_cols), BF),
            pltpu.VMEM((rows, gate_cols), F32),
            pltpu.VMEM((rows, state_cols), F32),
            pltpu.VMEM((n, rows, gate_cols), BF),
            pltpu.VMEM((n, rows, state_cols), BF),
            pltpu.VMEM((rows, gate_cols), F32),
            pltpu.VMEM((rows, state_cols), F32),
            pltpu.SemaphoreType.DMA((n,)),
            pltpu.SemaphoreType.DMA((4,)),
            pltpu.SemaphoreType.DMA((n,)),
            pltpu.SemaphoreType.DMA((n,)),
        ],
        name="apply_update",
    )(order, *sums, parts, dirs, gate_weight, state_weight, weights, *pieces)


def quick(n_fs, n_tp):
    def per_device(
        inputs, gate_cot, state_cot, gate_weight, state_weight, gate_factor, state_factor,
        gate_first, gate_second, state_first, state_second,
    ):
        fs = lax.axis_index("fs")
        tp = lax.axis_index("tp")
        rows = gate_factor.shape[0]
        rank = gate_factor.shape[1]
        tokens = inputs.shape[0]
        gate_cols = gate_cot.shape[1]
        state_cols = state_cot.shape[1]
        cols = gate_cols + state_cols
        quarter = 2 * rank // n_tp
        half = n_tp // 2
        own_rows = rank // n_fs

        all_weights = lax.all_gather(gate_weight.astype(BF), "fs", axis=0, tiled=True)

        factors = jnp.concatenate([gate_factor, state_factor], 1)
        mine = lax.dynamic_slice_in_dim(factors, tp * quarter, quarter, 1)
        got = {0: mine}
        for step in range(1, n_fs):
            got[step] = hop(mine, "fs", n_fs, step)
        order = jnp.stack([fs ^ step for step in range(n_fs)]).astype(jnp.int32)

        small = state_weight.astype(BF)
        small, got[n_fs - 1] = lax.optimization_barrier((small, got[n_fs - 1]))
        smalls = {0: small}
        for step in range(2, n_fs, 2):
            smalls[step] = hop(small, "fs", n_fs, step)
        for step in range(0, n_fs, 2):
            smalls[step + 1] = hop(smalls[step], "fs", n_fs, 1)

        lifted, part = lift(order, inputs, [got[step] for step in range(n_fs)])
        spread = {0: lifted}
        step = half
        while step:
            for known in list(spread):
                spread[known ^ step] = hop(spread[known], "tp", n_tp, step)
            step //= 2
        lifts = by_blocks(spread, n_tp)(tp)
        lifts, part = lax.optimization_barrier((lifts, part))

        gate_part = jnp.einsum("art,tc->arc", lifts[:half], gate_cot, preferred_element_type=F32)
        state_part = jnp.einsum("art,tc->arc", lifts[half:], state_cot, preferred_element_type=F32)
        partial = jnp.concatenate(
            [gate_part.reshape(n_fs, own_rows, gate_cols), state_part.reshape(n_fs, own_rows, state_cols)], 2
        )
        narrow = partial.astype(BF)
        projection = lax.dynamic_index_in_dim(partial, fs, 0, keepdims=False)
        for step in range(1, n_fs):
            sent = lax.dynamic_index_in_dim(narrow, fs ^ step, 0, keepdims=False)
            projection = projection + hop(sent, "fs", n_fs, step).astype(F32)

        def moments(first, second, proj):
            first_new = 0.8 * first + 0.2 * proj
            second_new = 0.9 * second + 0.1 * proj * proj
            return first_new, second_new, (first_new / jnp.sqrt(second_new)).astype(BF)

        gate_first_new, gate_second_new, gate_dir = moments(gate_first, gate_second, projection[:, :gate_cols])
        state_first_new, state_second_new, state_dir = moments(state_first, state_second, projection[:, gate_cols:])
        direction = jnp.concatenate([gate_dir, state_dir], 1)
        got = {0: direction}
        for step in range(1, n_fs):
            got[step] = hop(direction, "fs", n_fs, step)

        parts = [part] + [hop(part, "tp", n_tp, step) for step in range(1, n_tp)]
        tp_order = jnp.stack([tp ^ step for step in range(n_tp)]).astype(jnp.int32)

        dirs = by_blocks(got, n_fs)(fs).reshape(rank, cols)
        sums, all_parts = square_sums(tp_order, parts, dirs, gate_cols, rows)
        all_sums = [sums] + [hop(sums, "tp", n_tp, step) for step in range(1, n_tp)]
        d = n_fs * rows * n_tp
        gate_new, state_new, gate_copy, state_copy = apply_update(
            order, all_sums, all_parts, dirs, gate_weight, state_weight,
            all_weights, [smalls[step] for step in range(n_fs)], (d * gate_cols, d * state_cols),
        )
        return (
            gate_new, state_new, gate_copy, state_copy,
            gate_first_new, gate_second_new, state_first_new, state_second_new,
        )

    return per_device


def plain(n_fs, n_tp):
    def per_device(
        inputs, gate_cot, state_cot, gate_weight, state_weight, gate_factor, state_factor,
        gate_first, gate_second, state_first, state_second,
    ):
        def update(cot, weight, factor, first, second):
            whole = lax.all_gather(factor, "fs", axis=0, tiled=True)
            lifted = jnp.dot(inputs, whole, preferred_element_type=F32)
            upper = lifted.astype(BF)
            lower = (lifted - upper.astype(F32)).astype(BF)
            part = jnp.einsum("tr,tc->rc", upper, cot, preferred_element_type=F32)
            part = part + jnp.einsum("tr,tc->rc", lower, cot, preferred_element_type=F32)
            proj = lax.psum_scatter(part, "fs", scatter_dimension=0, tiled=True)
            first_new = 0.8 * first + 0.2 * proj
            second_new = 0.9 * second + 0.1 * proj * proj
            direction = (first_new / jnp.sqrt(second_new)).astype(BF)
            dirs = lax.all_gather(direction, "fs", axis=0, tiled=True)
            full = jnp.dot(factor, dirs, preferred_element_type=F32)
            square = lax.psum(jnp.sum(full * full), ("fs", "tp"))
            entries = full.shape[0] * full.shape[1] * n_fs * n_tp
            new = weight - 0.02 / jnp.sqrt(square / entries + 0.25) * full
            return new, lax.all_gather(new.astype(BF), "fs", axis=0, tiled=True), first_new, second_new

        g_new, g_copy, g_first, g_second = update(gate_cot, gate_weight, gate_factor, gate_first, gate_second)
        s_new, s_copy, s_first, s_second = update(state_cot, state_weight, state_factor, state_first, state_second)
        return g_new, s_new, g_copy, s_copy, g_first, g_second, s_first, s_second

    return per_device


def solution(mesh):
    n_fs = mesh.shape["fs"]
    n_tp = mesh.shape["tp"]
    small = n_fs in (2, 4, 8) and n_tp in (2, 4)
    both = P("fs", "tp")
    rows = P("fs", None)
    whole = P(None, "tp")
    return jax.shard_map(
        (quick if small else plain)(n_fs, n_tp),
        mesh=mesh,
        in_specs=(rows, both, both, both, both, rows, rows, both, both, both, both),
        out_specs=(both, both, whole, whole, both, both, both, both),
        check_vma=False,
    )
```
